32 devices in a mesh: grp: 2 (over x), tp: 16 (over z, y, core).
Axes of the slice: x: 2, y: 2, z: 4, core: 2. Of those that a mesh axis runs over, the one named last changes fastest.
Arguments:
- tokens: bfloat16 [128, 2048], P('grp'), parts along dimension 0, may hold values from -6 to 6
- norm_gain: float32 [2, 2048], replicated, may hold values from 0.1 to 1.9
- query_weight: bfloat16 [2, 2048, 2048], P(None, 'tp'), may hold values from -0.125 to 0.125
- key_weight: bfloat16 [2, 2048, 2048], P(None, 'tp'), may hold values from -0.125 to 0.125
- value_weight: bfloat16 [2, 2048, 2048], P(None, 'tp'), may hold values from -0.125 to 0.125
- outgate_weight: bfloat16 [2, 2048, 2048], P(None, 'tp'), may hold values from -0.125 to 0.125
- gate_weight: bfloat16 [2, 2048, 16], replicated, may hold values from -0.125 to 0.125
- forget_bias: float32 [2, 8], replicated, may hold values from 0 to 4
- proj_weight: bfloat16 [2, 2048, 2048], P(None, 'tp'), may hold values from -0.125 to 0.125
- cell_state: float32 [2, 128, 2048, 256], P(None, 'grp', 'tp'), parts along dimension 1, may hold values from -0.3 to 0.3
- normalizer: float32 [2, 128, 2048], P(None, 'grp', 'tp'), parts along dimension 1, may hold values from -0.3 to 0.3
- stabilizer: float32 [2, 128, 8], P(None, 'grp'), parts along dimension 1, may hold values from -2 to 2
Outputs:
- mixed: bfloat16 [128, 2048], P('grp', 'tp'), parts along dimension 0
- new_cell: float32 [2, 128, 2048, 256], P(None, 'grp', 'tp'), parts along dimension 1
- new_normalizer: float32 [2, 128, 2048], P(None, 'grp', 'tp'), parts along dimension 1
- new_stabilizer: float32 [2, 128, 8], P(None, 'grp'), parts along dimension 1
The draws below stay inside these ranges and needn't reach their ends.
There are 2 independent parts, one for each index of `grp`. The reference program is written for one: setup_inputs(seed, part) draws one part's arguments, and reference() takes and returns one part's arrays. A program takes and returns all parts, laid end to end along the dimension named above; an argument that names none is the same for every part. Nothing has to cross between parts.
All inputs are finite; a program needn't handle non-finite values.
Results may differ from the reference program's by a relative error of at most 0.025.
Values may be sent and summed in bfloat16 or wider, within the bound.
A program may use at most 64 MiB of HBM per device.

```python
import jax
import jax.numpy as jnp
from jax import lax

D = 2048
DH = 256
HEADS = 8
LAYERS = 2
BATCH = 64


def block_levels(rng, dims, split, low, largest):
    loudness = 1.0
    for axis_at, parts in split:
        heights = jax.random.uniform(jax.random.fold_in(jax.random.fold_in(rng, 6), axis_at), (parts,), jnp.float32, low / len(split), largest / len(split))
        loudness = loudness * jnp.repeat(jnp.exp(heights), dims[axis_at] // parts).reshape((-1,) + (1,) * (len(dims) - 1 - axis_at))
    return loudness


def centred(key, shape, width, most, shards=(), kind=jnp.bfloat16):
    entries = jax.random.normal(key, shape, jnp.float32) * width
    if len(shards) > 0:
        entries = block_levels(key, shape, shards, -0.22, 0.18) * entries
    return jnp.clip(entries, min=-most, max=most).astype(kind)


def setup_inputs(seed: int = 0, part: int = 0) -> dict:
    key_list = jax.random.split(jax.random.key(seed), 13)
    own_keys = jax.random.split(jax.random.fold_in(key_list[12], part), 13)
    tokens = centred(own_keys[0], (BATCH, D), 1.0, 6.0)
    norm_gain = jnp.clip(1.0 + 0.18 * jax.random.normal(key_list[1], (LAYERS, D), jnp.float32), 0.1, 1.9)
    query_weight = centred(key_list[2], (LAYERS, D, D), D ** -0.5, 0.125, ((1, 16),))
    key_weight = centred(key_list[3], (LAYERS, D, D), D ** -0.5, 0.125, ((1, 16),))
    value_weight = centred(key_list[4], (LAYERS, D, D), D ** -0.5, 0.125, ((1, 16),))
    outgate_weight = centred(key_list[5], (LAYERS, D, D), D ** -0.5, 0.125, ((1, 16),))
    gate_weight = centred(key_list[6], (LAYERS, D, 2 * HEADS), D ** -0.5, 0.125)
    forget_bias = jnp.clip(jax.random.uniform(key_list[7], (LAYERS, HEADS), jnp.float32, 0.0, 4.0), 0.0, 4.0)
    proj_weight = centred(key_list[8], (LAYERS, D, D), D ** -0.5, 0.125, ((1, 16),))
    cell_state = centred(own_keys[9], (LAYERS, BATCH, D, DH), 0.05, 0.3, ((2, 16),), jnp.float32)
    normalizer = centred(own_keys[10], (LAYERS, BATCH, D), 0.05, 0.3, ((2, 16),), jnp.float32)
    stabilizer = jnp.clip(jax.random.uniform(own_keys[11], (LAYERS, BATCH, HEADS), jnp.float32, -2.0, 2.0), -2.0, 2.0)
    return {"tokens": tokens, "norm_gain": norm_gain, "query_weight": query_weight, "key_weight": key_weight, "value_weight": value_weight, "outgate_weight": outgate_weight, "gate_weight": gate_weight, "forget_bias": forget_bias, "proj_weight": proj_weight, "cell_state": cell_state, "normalizer": normalizer, "stabilizer": stabilizer}


epsilon = 1e-06

def project(normed, weight):
    return lax.dot_general(normed, weight, (((1,), (1,)), ((), ())), preferred_element_type=jnp.float32)

def one_cell(current, gain, w_query, w_key, w_value, w_outgate, w_gates, bias_forget, w_proj, cell, norm_vec, stab):
    batch = current.shape[0]
    heads = D // DH
    cur_f = current.astype(jnp.float32)
    normed = (cur_f * lax.rsqrt(lax.optimization_barrier(jnp.mean(cur_f * cur_f, axis=-1, keepdims=True)) + epsilon) * gain).astype(jnp.bfloat16)
    query = project(normed, w_query).astype(jnp.bfloat16)
    keys = (project(normed, w_key) * DH ** (-0.5)).astype(jnp.bfloat16)
    values = project(normed, w_value).astype(jnp.bfloat16)
    outgate = project(normed, w_outgate).astype(jnp.bfloat16)
    gates = jnp.dot(normed, w_gates, preferred_element_type=jnp.float32)
    in_gate = gates[:, :heads]
    log_forget = jax.nn.log_sigmoid(gates[:, heads:] + bias_forget)
    new_stab = jnp.maximum(log_forget + stab, in_gate)
    decay = jnp.exp(log_forget + stab - new_stab)
    weight_in = jnp.exp(in_gate - new_stab)
    q_heads = query.astype(jnp.float32).reshape(batch, heads, DH)
    k_heads = keys.astype(jnp.float32).reshape(batch, heads, DH)
    v_heads = values.astype(jnp.float32).reshape(batch, heads, DH)
    old_cell = cell.reshape(batch, heads, DH, DH)
    outer = v_heads[:, :, :, None] * k_heads[:, :, None, :]
    new_cell = decay[:, :, None, None] * old_cell + weight_in[:, :, None, None] * outer
    new_norm = decay[:, :, None] * norm_vec.reshape(batch, heads, DH) + weight_in[:, :, None] * k_heads
    numer = jnp.einsum('bhk,bhek->bhe', q_heads, new_cell, precision=lax.Precision.HIGHEST)
    denom = lax.optimization_barrier(jnp.sum(q_heads * new_norm, axis=-1))
    readout = numer / jnp.maximum(jnp.abs(denom), jnp.exp(-new_stab))[:, :, None]
    branch = (jax.nn.sigmoid(outgate.astype(jnp.float32)) * readout.reshape(batch, D)).astype(jnp.bfloat16)
    result = (cur_f + project(branch, w_proj)).astype(jnp.bfloat16)
    return (result, new_cell.reshape(batch, D, DH), new_norm.reshape(batch, D), new_stab)

def reference(tokens, norm_gain, query_weight, key_weight, value_weight, outgate_weight, gate_weight, forget_bias, proj_weight, cell_state, normalizer, stabilizer):
    current = tokens
    cells = []
    norms = []
    stabs = []
    for layer in range(LAYERS):
        current, new_cell, new_norm, new_stab = one_cell(current, norm_gain[layer], query_weight[layer], key_weight[layer], value_weight[layer], outgate_weight[layer], gate_weight[layer], forget_bias[layer], proj_weight[layer], cell_state[layer], normalizer[layer], stabilizer[layer])
        cells.append(new_cell)
        norms.append(new_norm)
        stabs.append(new_stab)
    return (current, jnp.stack(cells), jnp.stack(norms), jnp.stack(stabs))
```

```python
import functools

import jax
import jax.numpy as jnp
from jax import lax
from jax.experimental import pallas as pl
from jax.experimental.pallas import tpu as pltpu
from jax.sharding import PartitionSpec as P

D = 2048
DH = 256
LAYERS = 2


epsilon = 1e-06


def from_partner(value, axis, apart):
    mask = 2**apart
    pairs = [(source, source ^ mask) for source in range(lax.axis_size(axis))]
    return lax.ppermute(value, axis, pairs)


def project(normed, weight):
    return lax.dot_general(
        normed, weight, (((1,), (1,)), ((), ())), preferred_element_type=jnp.float32
    )


def split_pieces(value):
    high = lax.optimization_barrier(value.astype(jnp.bfloat16))
    rest = value - high.astype(jnp.float32)
    middle = lax.optimization_barrier(rest.astype(jnp.bfloat16))
    lowest = (rest - middle.astype(jnp.float32)).astype(jnp.bfloat16)
    return jnp.stack([high, middle, lowest], axis=1)


def join_pieces(pieces):
    return jnp.sum(pieces.astype(jnp.float32), axis=-1)


def combine_halves(mine, theirs, lower):
    return jnp.where(
        lower, jnp.concatenate([mine, theirs], axis=1), jnp.concatenate([theirs, mine], axis=1)
    )


def one_cell(
    current,
    gain,
    w_query,
    w_key,
    w_value,
    w_outgate,
    w_gates,
    bias_forget,
    w_proj,
    cell,
    norm_vec,
    stab,
):
    heads = D // DH
    ncols = w_query.shape[0]
    group = DH // ncols
    device = lax.axis_index("tp")
    head = device // group
    cur_f = current.astype(jnp.float32)
    normed = (
        cur_f * lax.rsqrt(jnp.mean(cur_f * cur_f, axis=-1, keepdims=True) + epsilon) * gain
    ).astype(jnp.bfloat16)
    query = project(normed, w_query).astype(jnp.bfloat16)
    keys = (project(normed, w_key) * DH ** (-0.5)).astype(jnp.bfloat16)
    values = project(normed, w_value).astype(jnp.bfloat16)
    outgate = project(normed, w_outgate).astype(jnp.bfloat16)
    gates = jnp.dot(normed, w_gates, preferred_element_type=jnp.float32)
    in_gate = gates[:, :heads]
    log_forget = jax.nn.log_sigmoid(gates[:, heads:] + bias_forget)
    new_stab = jnp.maximum(log_forget + stab, in_gate)
    decay = jnp.exp(log_forget + stab - new_stab)
    weight_in = jnp.exp(in_gate - new_stab)
    select = (jnp.arange(heads) == head).astype(jnp.float32)
    my_decay = jnp.sum(decay * select, axis=-1)
    my_weight = jnp.sum(weight_in * select, axis=-1)
    my_stab = jnp.sum(new_stab * select, axis=-1)
    new_norm = my_decay[:, None] * norm_vec + my_weight[:, None] * keys.astype(jnp.float32)
    den_part = jnp.sum(query.astype(jnp.float32) * new_norm, axis=-1)
    q_head, k_head = (query, keys)
    denom = den_part
    for bit in range(group.bit_length() - 1):
        other_q, other_k, other_pieces = from_partner(
            (q_head, k_head, split_pieces(denom)), "tp", bit
        )
        lower = device // 2**bit % 2 == 0
        q_head = combine_halves(q_head, other_q, lower)
        k_head = combine_halves(k_head, other_k, lower)
        denom = denom + join_pieces(other_pieces)
    outer = values.astype(jnp.float32)[:, :, None] * k_head.astype(jnp.float32)[:, None, :]
    new_cell = my_decay[:, None, None] * cell + my_weight[:, None, None] * outer
    numer = jnp.einsum(
        "bk,bek->be", q_head.astype(jnp.float32), new_cell, precision=lax.Precision.HIGHEST
    )
    readout = numer / jnp.maximum(jnp.abs(denom), jnp.exp(-my_stab))[:, None]
    branch = (jax.nn.sigmoid(outgate.astype(jnp.float32)) * readout).astype(jnp.bfloat16)
    summed = project(lax.all_gather(branch, "tp", axis=1, tiled=True), w_proj)
    own_input = lax.dynamic_slice_in_dim(cur_f, device * ncols, ncols, 1)
    result = (own_input + summed).astype(jnp.bfloat16)
    return (result, new_cell, new_norm, new_stab)


def body(
    tokens,
    norm_gain,
    query_weight,
    key_weight,
    value_weight,
    outgate_weight,
    gate_weight,
    forget_bias,
    proj_weight,
    cell_state,
    normalizer,
    stabilizer,
):
    current = tokens
    cells = []
    norms = []
    stabs = []
    result = tokens
    for layer in range(LAYERS):
        result, new_cell, new_norm, new_stab = one_cell(
            current,
            norm_gain[layer],
            query_weight[layer],
            key_weight[layer],
            value_weight[layer],
            outgate_weight[layer],
            gate_weight[layer],
            forget_bias[layer],
            proj_weight[layer],
            cell_state[layer],
            normalizer[layer],
            stabilizer[layer],
        )
        cells.append(new_cell)
        norms.append(new_norm)
        stabs.append(new_stab)
        if layer + 1 < LAYERS:
            current = lax.all_gather(result, "tp", axis=1, tiled=True)
    return (result, jnp.stack(cells), jnp.stack(norms), jnp.stack(stabs))


NT = (((1,), (1,)), ((), ()))
CELL_CHUNKS = 4


def fused_kernel(
    n,
    group,
    tokens,
    norm_gain,
    w_query,
    w_key,
    w_value,
    w_outgate,
    w_gates,
    bias_forget,
    w_proj,
    cell,
    norm_vec,
    stab,
    mixed,
    cell_buf,
    new_norm,
    new_stab,
    wv_buf,
    key_buf,
    decay_buf,
    tok_buf,
    gain_buf,
    weights,
    gate_buf,
    bias_buf,
    stab_buf,
    norm_buf,
    pair_buf,
    branch_buf,
    result_buf,
    numer_buf,
    small_sem,
    weight_sem,
    cell_sem,
    norm_send,
    norm_recv,
    pair_send,
    pair_recv,
    gather_send,
    gather_recv,
):
    layers, batch, ncols, dh = cell.shape
    width = tokens.shape[1]
    heads = stab.shape[1]
    rows = batch // CELL_CHUNKS
    me = lax.axis_index("tp")
    place = lax.rem(me, group)
    first = me - place
    head = lax.div(me, group)
    barrier = pltpu.get_barrier_semaphore()
    for i in range(1, n):
        pl.semaphore_signal(
            barrier,
            inc=1,
            device_id={"tp": lax.rem(me + i, n)},
            device_id_type=pl.DeviceIdType.MESH,
        )

    def fetch(source, target, sem):
        copy = pltpu.make_async_copy(source, target, sem)
        copy.start()
        return copy

    small = [
        fetch(source, target, small_sem.at[i])
        for i, (source, target) in enumerate(
            [
                (tokens, tok_buf),
                (norm_gain, gain_buf),
                (w_gates, gate_buf),
                (bias_forget, bias_buf),
                (stab, stab_buf),
            ]
        )
    ]
    norm_copy = fetch(norm_vec, norm_buf.at[place], small_sem.at[5])
    names = [w_query, w_key, w_value, w_outgate, w_proj]
    weight_copies = [[None] * 5 for _ in range(layers)]
    cell_copies = [[None] * CELL_CHUNKS for _ in range(layers)]
    for layer in range(layers):
        for i in range(4):
            weight_copies[layer][i] = fetch(
                names[i].at[layer],
                weights.at[layer, pl.ds(i * ncols, ncols)],
                weight_sem.at[layer, i],
            )
        for c in range(CELL_CHUNKS):
            part = pl.ds(c * rows, rows)
            cell_copies[layer][c] = fetch(
                cell.at[layer, part], cell_buf.at[layer, part], cell_sem.at[layer, c]
            )
        weight_copies[layer][4] = fetch(
            names[4].at[layer],
            weights.at[layer, pl.ds(4 * ncols, ncols)],
            weight_sem.at[layer, 4],
        )

    def to_group(source, send, recv):
        copies = []
        for i in range(1, group):
            copy = pltpu.make_async_remote_copy(
                src_ref=source.at[place],
                dst_ref=source.at[place],
                send_sem=send.at[i],
                recv_sem=recv.at[i],
                device_id={"tp": first + lax.rem(place + i, group)},
                device_id_type=pl.DeviceIdType.MESH,
            )
            copy.start()
            copies.append(copy)
        return copies

    def finish_group(copies, source, recv):
        for i, copy in enumerate(copies, 1):
            origin = lax.rem(place + group - i, group)
            pltpu.make_async_copy(source.at[origin], source.at[origin], recv.at[i]).wait()
            copy.wait_send()

    def to_all(buffer, send, recv):
        copies = []
        for i in range(1, n):
            copy = pltpu.make_async_remote_copy(
                src_ref=buffer.at[me],
                dst_ref=buffer.at[me],
                send_sem=send.at[i],
                recv_sem=recv.at[i],
                device_id={"tp": lax.rem(me + i, n)},
                device_id_type=pl.DeviceIdType.MESH,
            )
            copy.start()
            copies.append(copy)
        return copies

    def finish_all(copies, buffer, recv):
        for i, copy in enumerate(copies, 1):
            origin = lax.rem(me + n - i, n)
            pltpu.make_async_copy(buffer.at[origin], buffer.at[origin], recv.at[i]).wait()
            copy.wait_send()

    for copy in small:
        copy.wait()
    norm_copies = None
    own = tok_buf[:, pl.ds(pl.multiple_of(me * ncols, ncols), ncols)].astype(jnp.float32)
    for layer in range(layers):
        if layer == 0:
            current = tok_buf[...].astype(jnp.float32)
        else:
            current = jnp.concatenate(
                [result_buf[layer - 1, d] for d in range(n)], axis=1
            ).astype(jnp.float32)
        mean = jnp.sum(current * current, axis=-1, keepdims=True) * (1.0 / width)
        normed = (current * lax.rsqrt(mean + epsilon) * gain_buf[pl.ds(layer, 1), :]).astype(
            jnp.bfloat16
        )
        for i in range(4):
            weight_copies[layer][i].wait()
        both = lax.dot_general(
            normed, weights[layer, : 2 * ncols], NT, preferred_element_type=jnp.float32
        )
        query = both[:, :ncols].astype(jnp.bfloat16)
        key = (both[:, ncols:] * dh ** (-0.5)).astype(jnp.bfloat16)
        pair_buf[layer, place, 0] = query
        pair_buf[layer, place, 1] = key
        if layer == 0:
            norm_copy.wait()
            pl.semaphore_wait(barrier, n - 1)
        pair_copies = to_group(pair_buf.at[layer], pair_send.at[layer], pair_recv.at[layer])
        if layer == 0:
            norm_copies = to_group(norm_buf, norm_send, norm_recv)
        both = lax.dot_general(
            normed,
            weights[layer, 2 * ncols : 4 * ncols],
            NT,
            preferred_element_type=jnp.float32,
        )
        value = both[:, :ncols].astype(jnp.bfloat16).astype(jnp.float32)
        outgate = both[:, ncols:].astype(jnp.bfloat16).astype(jnp.float32)
        gates = lax.dot_general(
            normed, gate_buf[layer], NT, preferred_element_type=jnp.float32
        )
        in_gate = gates[:, :heads]
        forget = gates[:, heads:] + bias_buf[pl.ds(layer, 1), :]
        log_forget = jnp.minimum(forget, 0.0) - jnp.log1p(jnp.exp(-jnp.abs(forget)))
        old_stab = stab_buf[layer].T
        next_stab = jnp.maximum(log_forget + old_stab, in_gate)
        new_stab[layer] = next_stab.T
        mine = lax.broadcasted_iota(jnp.int32, (batch, heads), 1) == head

        def pick(entry):
            return jnp.sum(jnp.where(mine, entry, 0.0), axis=-1, keepdims=True)

        my_stab = pick(next_stab)
        my_decay = jnp.exp(pick(log_forget + old_stab) - my_stab)
        my_weight = jnp.exp(pick(in_gate) - my_stab)
        new_norm[layer] = my_decay * norm_buf[place, layer] + my_weight * key.astype(jnp.float32)
        weighted = my_weight * value
        wv_buf[layer] = weighted
        decay_buf[layer] = jnp.broadcast_to(my_decay, (batch, ncols))
        gate = jax.nn.sigmoid(outgate)

        finish_group(pair_copies, pair_buf.at[layer], pair_recv.at[layer])
        if layer == 0:
            finish_group(norm_copies, norm_buf, norm_recv)
        q_head = jnp.concatenate([pair_buf[layer, j, 0] for j in range(group)], axis=1)
        q_head = q_head.astype(jnp.float32)
        k_head = jnp.concatenate([pair_buf[layer, j, 1] for j in range(group)], axis=1)
        k_head = k_head.astype(jnp.float32)
        n_head = jnp.concatenate([norm_buf[j, layer] for j in range(group)], axis=1)
        key_buf[layer] = k_head
        denom = jnp.sum(
            q_head * (my_decay * n_head + my_weight * k_head), axis=-1, keepdims=True
        )
        inner = jnp.sum(q_head * k_head, axis=-1, keepdims=True)

        def read_rows(c, start, layer=layer):
            queries = jnp.concatenate(
                [pair_buf[layer, j, 0, pl.ds(start, rows), :] for j in range(group)], axis=1
            )
            row = lax.broadcasted_iota(jnp.int32, (rows, ncols), 0)
            total = jnp.zeros((rows, ncols), jnp.float32)
            for b in range(rows):
                block = cell_buf[layer, start + b].astype(jnp.bfloat16)
                product = lax.dot_general(
                    queries, block, NT, preferred_element_type=jnp.float32
                )
                total = jnp.where(row == b, product, total)
            numer_buf[pl.ds(start, rows), :] = total

        for c in range(CELL_CHUNKS):
            cell_copies[layer][c].wait()
            read_rows(c, c * rows)
        numer = my_decay * numer_buf[...] + weighted * inner
        readout = numer / jnp.maximum(jnp.abs(denom), jnp.exp(-my_stab))
        branch_buf[layer, me] = (gate * readout).astype(jnp.bfloat16)
        branch_copies = to_all(
            branch_buf.at[layer], gather_send.at[layer, 0], gather_recv.at[layer, 0]
        )

        weight_copies[layer][4].wait()
        finish_all(branch_copies, branch_buf.at[layer], gather_recv.at[layer, 0])
        branch = jnp.concatenate([branch_buf[layer, d] for d in range(n)], axis=1)
        summed = lax.dot_general(
            branch,
            weights[layer, 4 * ncols : 5 * ncols],
            NT,
            preferred_element_type=jnp.float32,
        )
        result = (own + summed).astype(jnp.bfloat16)
        own = result.astype(jnp.float32)
        if layer + 1 < layers:
            result_buf[layer, me] = result
            result_copies = to_all(
                result_buf.at[layer], gather_send.at[layer, 1], gather_recv.at[layer, 1]
            )
            finish_all(result_copies, result_buf.at[layer], gather_recv.at[layer, 1])
        else:
            mixed[...] = result


def fused_body(n, *args):
    (tokens, norm_gain, w_query, _, _, _, w_gates, bias_forget, _, cell, norm_vec, stab) = args
    layers, batch, ncols, dh = cell.shape
    width = tokens.shape[1]
    group = dh // ncols
    w_gates = jnp.swapaxes(w_gates, 1, 2)
    stab = jnp.swapaxes(stab, 1, 2)
    args = args[:6] + (w_gates,) + args[7:11] + (stab,)
    args = [pltpu.with_memory_space_constraint(arg, pltpu.HBM) for arg in args]
    bf16, f32 = jnp.bfloat16, jnp.float32
    vmem = pl.BlockSpec(memory_space=pltpu.VMEM)
    dma = pltpu.SemaphoreType.DMA
    mixed, held, new_norm, new_stab, weighted, keys, decay = pl.pallas_call(
        functools.partial(fused_kernel, n, group),
        out_shape=(
            jax.ShapeDtypeStruct((batch, ncols), bf16),
            pltpu.VMEM(cell.shape, f32),
            jax.ShapeDtypeStruct(norm_vec.shape, f32),
            jax.ShapeDtypeStruct(stab.shape, f32),
            jax.ShapeDtypeStruct((layers, batch, ncols), f32),
            jax.ShapeDtypeStruct((layers, batch, dh), f32),
            jax.ShapeDtypeStruct((layers, batch, ncols), f32),
        ),
        in_specs=[pl.BlockSpec(memory_space=pltpu.HBM)] * len(args),
        out_specs=(vmem,) * 7,
        scratch_shapes=[
            pltpu.VMEM(tokens.shape, bf16),
            pltpu.VMEM(norm_gain.shape, f32),
            pltpu.VMEM((layers, 5 * ncols, width), bf16),
            pltpu.VMEM(w_gates.shape, bf16),
            pltpu.VMEM(bias_forget.shape, f32),
            pltpu.VMEM(stab.shape, f32),
            pltpu.VMEM((group,) + norm_vec.shape, f32),
            pltpu.VMEM((layers, group, 2, batch, ncols), bf16),
            pltpu.VMEM((layers, n, batch, ncols), bf16),
            pltpu.VMEM((layers, n, batch, ncols), bf16),
            pltpu.VMEM((batch, ncols), f32),
            dma((6,)),
            dma((layers, 5)),
            dma((layers, CELL_CHUNKS)),
            dma((group,)),
            dma((group,)),
            dma((layers, group)),
            dma((layers, group)),
            dma((layers, 2, n)),
            dma((layers, 2, n)),
        ],
        compiler_params=pltpu.CompilerParams(
            collective_id=0, has_side_effects=True, vmem_limit_bytes=VMEM_LIMIT
        ),
        name="cells",
    )(*args)
    new_cell = (
        decay[:, :, :1, None] * held + weighted[:, :, :, None] * keys[:, :, None, :]
    )
    return mixed, new_cell, new_norm, jnp.swapaxes(new_stab, 1, 2)


VMEM_LIMIT = 24 * 2**20


def whole_body(*args):
    n = lax.axis_size("tp")
    _, batch, ncols, dh = args[9].shape
    if ncols % 128 == 0 and dh % ncols == 0 and batch % (16 * CELL_CHUNKS) == 0:
        return fused_body(n, *args)
    return body(*args)


def solution(mesh):
    return jax.shard_map(
        whole_body,
        mesh=mesh,
        in_specs=(
            P("grp", None),
            P(),
            P(None, "tp", None),
            P(None, "tp", None),
            P(None, "tp", None),
            P(None, "tp", None),
            P(),
            P(),
            P(None, "tp", None),
            P(None, "grp", "tp", None),
            P(None, "grp", "tp"),
            P(None, "grp", None),
        ),
        out_specs=(
            P("grp", "tp"),
            P(None, "grp", "tp", None),
            P(None, "grp", "tp"),
            P(None, "grp", None),
        ),
        check_vma=False,
    )
```

```python
import functools

import jax
import jax.numpy as jnp
from jax import lax
from jax.experimental import pallas as pl
from jax.experimental.pallas import tpu as pltpu
from jax.sharding import PartitionSpec as P

D = 2048
DH = 256
LAYERS = 2


epsilon = 1e-06


def from_partner(value, axis, apart):
    mask = 2**apart
    pairs = [(source, source ^ mask) for source in range(lax.axis_size(axis))]
    return lax.ppermute(value, axis, pairs)


def project(normed, weight):
    return lax.dot_general(
        normed, weight, (((1,), (1,)), ((), ())), preferred_element_type=jnp.float32
    )


def split_pieces(value):
    high = lax.optimization_barrier(value.astype(jnp.bfloat16))
    rest = value - high.astype(jnp.float32)
    middle = lax.optimization_barrier(rest.astype(jnp.bfloat16))
    lowest = (rest - middle.astype(jnp.float32)).astype(jnp.bfloat16)
    return jnp.stack([high, middle, lowest], axis=1)


def join_pieces(pieces):
    return jnp.sum(pieces.astype(jnp.float32), axis=-1)


def combine_halves(mine, theirs, lower):
    return jnp.where(
        lower, jnp.concatenate([mine, theirs], axis=1), jnp.concatenate([theirs, mine], axis=1)
    )


def one_cell(
    current,
    gain,
    w_query,
    w_key,
    w_value,
    w_outgate,
    w_gates,
    bias_forget,
    w_proj,
    cell,
    norm_vec,
    stab,
):
    heads = D // DH
    ncols = w_query.shape[0]
    group = DH // ncols
    device = lax.axis_index("tp")
    head = device // group
    cur_f = current.astype(jnp.float32)
    normed = (
        cur_f * lax.rsqrt(jnp.mean(cur_f * cur_f, axis=-1, keepdims=True) + epsilon) * gain
    ).astype(jnp.bfloat16)
    query = project(normed, w_query).astype(jnp.bfloat16)
    keys = (project(normed, w_key) * DH ** (-0.5)).astype(jnp.bfloat16)
    values = project(normed, w_value).astype(jnp.bfloat16)
    outgate = project(normed, w_outgate).astype(jnp.bfloat16)
    gates = jnp.dot(normed, w_gates, preferred_element_type=jnp.float32)
    in_gate = gates[:, :heads]
    log_forget = jax.nn.log_sigmoid(gates[:, heads:] + bias_forget)
    new_stab = jnp.maximum(log_forget + stab, in_gate)
    decay = jnp.exp(log_forget + stab - new_stab)
    weight_in = jnp.exp(in_gate - new_stab)
    select = (jnp.arange(heads) == head).astype(jnp.float32)
    my_decay = jnp.sum(decay * select, axis=-1)
    my_weight = jnp.sum(weight_in * select, axis=-1)
    my_stab = jnp.sum(new_stab * select, axis=-1)
    new_norm = my_decay[:, None] * norm_vec + my_weight[:, None] * keys.astype(jnp.float32)
    den_part = jnp.sum(query.astype(jnp.float32) * new_norm, axis=-1)
    q_head, k_head = (query, keys)
    denom = den_part
    for bit in range(group.bit_length() - 1):
        other_q, other_k, other_pieces = from_partner(
            (q_head, k_head, split_pieces(denom)), "tp", bit
        )
        lower = device // 2**bit % 2 == 0
        q_head = combine_halves(q_head, other_q, lower)
        k_head = combine_halves(k_head, other_k, lower)
        denom = denom + join_pieces(other_pieces)
    outer = values.astype(jnp.float32)[:, :, None] * k_head.astype(jnp.float32)[:, None, :]
    new_cell = my_decay[:, None, None] * cell + my_weight[:, None, None] * outer
    numer = jnp.einsum(
        "bk,bek->be", q_head.astype(jnp.float32), new_cell, precision=lax.Precision.HIGHEST
    )
    readout = numer / jnp.maximum(jnp.abs(denom), jnp.exp(-my_stab))[:, None]
    branch = (jax.nn.sigmoid(outgate.astype(jnp.float32)) * readout).astype(jnp.bfloat16)
    summed = project(lax.all_gather(branch, "tp", axis=1, tiled=True), w_proj)
    own_input = lax.dynamic_slice_in_dim(cur_f, device * ncols, ncols, 1)
    result = (own_input + summed).astype(jnp.bfloat16)
    return (result, new_cell, new_norm, new_stab)


def body(
    tokens,
    norm_gain,
    query_weight,
    key_weight,
    value_weight,
    outgate_weight,
    gate_weight,
    forget_bias,
    proj_weight,
    cell_state,
    normalizer,
    stabilizer,
):
    current = tokens
    cells = []
    norms = []
    stabs = []
    result = tokens
    for layer in range(LAYERS):
        result, new_cell, new_norm, new_stab = one_cell(
            current,
            norm_gain[layer],
            query_weight[layer],
            key_weight[layer],
            value_weight[layer],
            outgate_weight[layer],
            gate_weight[layer],
            forget_bias[layer],
            proj_weight[layer],
            cell_state[layer],
            normalizer[layer],
            stabilizer[layer],
        )
        cells.append(new_cell)
        norms.append(new_norm)
        stabs.append(new_stab)
        if layer + 1 < LAYERS:
            current = lax.all_gather(result, "tp", axis=1, tiled=True)
    return (result, jnp.stack(cells), jnp.stack(norms), jnp.stack(stabs))


NT = (((1,), (1,)), ((), ()))
CELL_CHUNKS = 4


def fused_kernel(
    n,
    group,
    tokens,
    norm_gain,
    w_query,
    w_key,
    w_value,
    w_outgate,
    w_gates,
    bias_forget,
    w_proj,
    cell,
    norm_vec,
    stab,
    mixed,
    cell_buf,
    new_norm,
    new_stab,
    wv_buf,
    key_buf,
    decay_buf,
    tok_buf,
    gain_buf,
    weights,
    gate_buf,
    bias_buf,
    stab_buf,
    norm_buf,
    pair_buf,
    branch_buf,
    result_buf,
    numer_buf,
    small_sem,
    weight_sem,
    cell_sem,
    norm_send,
    norm_recv,
    pair_send,
    pair_recv,
    gather_send,
    gather_recv,
):
    layers, batch, ncols, dh = cell.shape
    width = tokens.shape[1]
    heads = stab.shape[1]
    rows = batch // CELL_CHUNKS
    me = lax.axis_index("tp")
    place = lax.rem(me, group)
    first = me - place
    head = lax.div(me, group)
    barrier = pltpu.get_barrier_semaphore()
    for i in range(1, n):
        pl.semaphore_signal(
            barrier,
            inc=1,
            device_id={"tp": lax.rem(me + i, n)},
            device_id_type=pl.DeviceIdType.MESH,
        )

    def fetch(source, target, sem):
        copy = pltpu.make_async_copy(source, target, sem)
        copy.start()
        return copy

    small = [
        fetch(source, target, small_sem.at[i])
        for i, (source, target) in enumerate(
            [
                (tokens, tok_buf),
                (norm_gain, gain_buf),
                (w_gates, gate_buf),
                (bias_forget, bias_buf),
                (stab, stab_buf),
            ]
        )
    ]
    norm_copy = fetch(norm_vec, norm_buf.at[place], small_sem.at[5])
    names = [w_query, w_key, w_value, w_outgate, w_proj]
    weight_copies = [[None] * 5 for _ in range(layers)]
    cell_copies = [[None] * CELL_CHUNKS for _ in range(layers)]

    def fetch_weights(layer):
        for i in range(4):
            weight_copies[layer][i] = fetch(
                names[i].at[layer],
                weights.at[layer, pl.ds(i * ncols, ncols)],
                weight_sem.at[layer, i],
            )

    def fetch_cell(layer):
        for c in range(CELL_CHUNKS):
            part = pl.ds(c * rows, rows)
            cell_copies[layer][c] = fetch(
                cell.at[layer, part], cell_buf.at[layer, part], cell_sem.at[layer, c]
            )
        weight_copies[layer][4] = fetch(
            names[4].at[layer],
            weights.at[layer, pl.ds(4 * ncols, ncols)],
            weight_sem.at[layer, 4],
        )

    fetch_weights(0)

    def to_group(source, send, recv):
        copies = []
        for i in range(1, group):
            copy = pltpu.make_async_remote_copy(
                src_ref=source.at[place],
                dst_ref=source.at[place],
                send_sem=send.at[i],
                recv_sem=recv.at[i],
                device_id={"tp": first + lax.rem(place + i, group)},
                device_id_type=pl.DeviceIdType.MESH,
            )
            copy.start()
            copies.append(copy)
        return copies

    def finish_group(copies, source, recv):
        for i, copy in enumerate(copies, 1):
            origin = lax.rem(place + group - i, group)
            pltpu.make_async_copy(source.at[origin], source.at[origin], recv.at[i]).wait()
            copy.wait_send()

    chips = n // 2
    core = lax.rem(me, 2)
    chip = lax.div(me, 2)

    def push(buffer, at, target, send, recv):
        copy = pltpu.make_async_remote_copy(
            src_ref=buffer.at[at],
            dst_ref=buffer.at[at],
            send_sem=send,
            recv_sem=recv,
            device_id={"tp": target},
            device_id_type=pl.DeviceIdType.MESH,
        )
        copy.start()
        return copy

    def to_all(buffer, send, recv):
        copies = [
            push(buffer, me, lax.rem(chip + i, chips) * 2 + core, send.at[0, i], recv.at[0, i])
            for i in range(1, chips)
        ]
        copies.append(push(buffer, me, chip * 2 + 1 - core, send.at[1, 0], recv.at[1, 0]))
        return copies

    def finish_all(copies, buffer, send, recv):
        for i in range(1, chips):
            origin = lax.rem(chip + chips - i, chips) * 2 + core
            pltpu.make_async_copy(buffer.at[origin], buffer.at[origin], recv.at[0, i]).wait()
            copies.append(
                push(buffer, origin, chip * 2 + 1 - core, send.at[1, i], recv.at[1, i])
            )
        for i in range(chips):
            origin = lax.rem(chip + chips - i, chips) * 2 + 1 - core
            pltpu.make_async_copy(buffer.at[origin], buffer.at[origin], recv.at[1, i]).wait()
        for copy in copies:
            copy.wait_send()

    for copy in small:
        copy.wait()
    norm_copies = None
    own = tok_buf[:, pl.ds(pl.multiple_of(me * ncols, ncols), ncols)].astype(jnp.float32)
    for layer in range(layers):
        if layer == 0:
            current = tok_buf[...].astype(jnp.float32)
        else:
            current = jnp.concatenate(
                [result_buf[layer - 1, d] for d in range(n)], axis=1
            ).astype(jnp.float32)
        mean = jnp.sum(current * current, axis=-1, keepdims=True) * (1.0 / width)
        normed = (current * lax.rsqrt(mean + epsilon) * gain_buf[pl.ds(layer, 1), :]).astype(
            jnp.bfloat16
        )
        for i in range(4):
            weight_copies[layer][i].wait()
        if layer == 0:
            fetch_cell(layer)
        both = lax.dot_general(
            normed, weights[layer, : 2 * ncols], NT, preferred_element_type=jnp.float32
        )
        query = both[:, :ncols].astype(jnp.bfloat16)
        key = (both[:, ncols:] * dh ** (-0.5)).astype(jnp.bfloat16)
        pair_buf[layer, place, 0] = query
        pair_buf[layer, place, 1] = key
        if layer == 0:
            norm_copy.wait()
            pl.semaphore_wait(barrier, n - 1)
        pair_copies = to_group(pair_buf.at[layer], pair_send.at[layer], pair_recv.at[layer])
        if layer == 0:
            norm_copies = to_group(norm_buf, norm_send, norm_recv)
        both = lax.dot_general(
            normed,
            weights[layer, 2 * ncols : 4 * ncols],
            NT,
            preferred_element_type=jnp.float32,
        )
        value = both[:, :ncols].astype(jnp.bfloat16).astype(jnp.float32)
        outgate = both[:, ncols:].astype(jnp.bfloat16).astype(jnp.float32)
        gates = lax.dot_general(
            normed, gate_buf[layer], NT, preferred_element_type=jnp.float32
        )
        in_gate = gates[:, :heads]
        forget = gates[:, heads:] + bias_buf[pl.ds(layer, 1), :]
        log_forget = jnp.minimum(forget, 0.0) - jnp.log1p(jnp.exp(-jnp.abs(forget)))
        old_stab = stab_buf[layer].T
        next_stab = jnp.maximum(log_forget + old_stab, in_gate)
        new_stab[layer] = next_stab.T
        mine = lax.broadcasted_iota(jnp.int32, (batch, heads), 1) == head

        def pick(entry):
            return jnp.sum(jnp.where(mine, entry, 0.0), axis=-1, keepdims=True)

        my_stab = pick(next_stab)
        my_decay = jnp.exp(pick(log_forget + old_stab) - my_stab)
        my_weight = jnp.exp(pick(in_gate) - my_stab)
        new_norm[layer] = my_decay * norm_buf[place, layer] + my_weight * key.astype(jnp.float32)
        weighted = my_weight * value
        wv_buf[layer] = weighted
        decay_buf[layer] = jnp.broadcast_to(my_decay, (batch, ncols))
        gate = jax.nn.sigmoid(outgate)

        finish_group(pair_copies, pair_buf.at[layer], pair_recv.at[layer])
        if layer == 0:
            finish_group(norm_copies, norm_buf, norm_recv)
        q_head = jnp.concatenate([pair_buf[layer, j, 0] for j in range(group)], axis=1)
        q_head = q_head.astype(jnp.float32)
        k_head = jnp.concatenate([pair_buf[layer, j, 1] for j in range(group)], axis=1)
        k_head = k_head.astype(jnp.float32)
        n_head = jnp.concatenate([norm_buf[j, layer] for j in range(group)], axis=1)
        key_buf[layer] = k_head
        denom = jnp.sum(
            q_head * (my_decay * n_head + my_weight * k_head), axis=-1, keepdims=True
        )
        inner = jnp.sum(q_head * k_head, axis=-1, keepdims=True)

        def read_rows(c, start, layer=layer):
            queries = jnp.concatenate(
                [pair_buf[layer, j, 0, pl.ds(start, rows), :] for j in range(group)], axis=1
            )
            row = lax.broadcasted_iota(jnp.int32, (rows, ncols), 0)
            total = jnp.zeros((rows, ncols), jnp.float32)
            for b in range(rows):
                block = cell_buf[layer, start + b].astype(jnp.bfloat16)
                product = lax.dot_general(
                    queries, block, NT, preferred_element_type=jnp.float32
                )
                total = jnp.where(row == b, product, total)
            numer_buf[pl.ds(start, rows), :] = total

        for c in range(CELL_CHUNKS):
            cell_copies[layer][c].wait()
            read_rows(c, c * rows)
        numer = my_decay * numer_buf[...] + weighted * inner
        readout = numer / jnp.maximum(jnp.abs(denom), jnp.exp(-my_stab))
        branch_buf[layer, me] = (gate * readout).astype(jnp.bfloat16)
        branch_copies = to_all(
            branch_buf.at[layer], gather_send.at[layer, 0], gather_recv.at[layer, 0]
        )
        if layer + 1 < layers:
            fetch_weights(layer + 1)
            fetch_cell(layer + 1)

        weight_copies[layer][4].wait()
        finish_all(
            branch_copies,
            branch_buf.at[layer],
            gather_send.at[layer, 0],
            gather_recv.at[layer, 0],
        )
        branch = jnp.concatenate([branch_buf[layer, d] for d in range(n)], axis=1)
        summed = lax.dot_general(
            branch,
            weights[layer, 4 * ncols : 5 * ncols],
            NT,
            preferred_element_type=jnp.float32,
        )
        result = (own + summed).astype(jnp.bfloat16)
        own = result.astype(jnp.float32)
        if layer + 1 < layers:
            result_buf[layer, me] = result
            result_copies = to_all(
                result_buf.at[layer], gather_send.at[layer, 1], gather_recv.at[layer, 1]
            )
            finish_all(
                result_copies,
                result_buf.at[layer],
                gather_send.at[layer, 1],
                gather_recv.at[layer, 1],
            )
        else:
            mixed[...] = result


def fused_body(n, *args):
    (tokens, norm_gain, w_query, _, _, _, w_gates, bias_forget, _, cell, norm_vec, stab) = args
    layers, batch, ncols, dh = cell.shape
    width = tokens.shape[1]
    group = dh // ncols
    w_gates = jnp.swapaxes(w_gates, 1, 2)
    stab = jnp.swapaxes(stab, 1, 2)
    args = args[:6] + (w_gates,) + args[7:11] + (stab,)
    args = [pltpu.with_memory_space_constraint(arg, pltpu.HBM) for arg in args]
    bf16, f32 = jnp.bfloat16, jnp.float32
    vmem = pl.BlockSpec(memory_space=pltpu.VMEM)
    dma = pltpu.SemaphoreType.DMA
    mixed, held, new_norm, new_stab, weighted, keys, decay = pl.pallas_call(
        functools.partial(fused_kernel, n, group),
        out_shape=(
            jax.ShapeDtypeStruct((batch, ncols), bf16),
            pltpu.VMEM(cell.shape, f32),
            jax.ShapeDtypeStruct(norm_vec.shape, f32),
            jax.ShapeDtypeStruct(stab.shape, f32),
            jax.ShapeDtypeStruct((layers, batch, ncols), f32),
            jax.ShapeDtypeStruct((layers, batch, dh), f32),
            jax.ShapeDtypeStruct((layers, batch, ncols), f32),
        ),
        in_specs=[pl.BlockSpec(memory_space=pltpu.HBM)] * len(args),
        out_specs=(vmem,) * 7,
        scratch_shapes=[
            pltpu.VMEM(tokens.shape, bf16),
            pltpu.VMEM(norm_gain.shape, f32),
            pltpu.VMEM((layers, 5 * ncols, width), bf16),
            pltpu.VMEM(w_gates.shape, bf16),
            pltpu.VMEM(bias_forget.shape, f32),
            pltpu.VMEM(stab.shape, f32),
            pltpu.VMEM((group,) + norm_vec.shape, f32),
            pltpu.VMEM((layers, group, 2, batch, ncols), bf16),
            pltpu.VMEM((layers, n, batch, ncols), bf16),
            pltpu.VMEM((layers, n, batch, ncols), bf16),
            pltpu.VMEM((batch, ncols), f32),
            dma((6,)),
            dma((layers, 5)),
            dma((layers, CELL_CHUNKS)),
            dma((group,)),
            dma((group,)),
            dma((layers, group)),
            dma((layers, group)),
            dma((layers, 2, 2, n // 2)),
            dma((layers, 2, 2, n // 2)),
        ],
        compiler_params=pltpu.CompilerParams(
            collective_id=0, has_side_effects=True, vmem_limit_bytes=VMEM_LIMIT
        ),
        name="cells",
    )(*args)
    new_cell = (
        decay[:, :, :1, None] * held + weighted[:, :, :, None] * keys[:, :, None, :]
    )
    mixed, new_norm, new_stab = write_small(mixed, new_norm, new_stab)
    return mixed, new_cell, new_norm, jnp.swapaxes(new_stab, 1, 2)


def write_kernel(*refs):
    half = len(refs) // 2
    sems = refs[-1]
    copies = [
        pltpu.make_async_copy(refs[i], refs[half + i], sems.at[i]) for i in range(half)
    ]
    for copy in copies:
        copy.start()
    for copy in copies:
        copy.wait()


def write_small(*arrays):
    return pl.pallas_call(
        write_kernel,
        out_shape=[jax.ShapeDtypeStruct(x.shape, x.dtype) for x in arrays],
        in_specs=[pl.BlockSpec(memory_space=pltpu.VMEM)] * len(arrays),
        out_specs=[pl.BlockSpec(memory_space=pltpu.HBM)] * len(arrays),
        scratch_shapes=[pltpu.SemaphoreType.DMA((len(arrays),))],
        compiler_params=pltpu.CompilerParams(vmem_limit_bytes=2**20),
        name="write",
    )(*arrays)


VMEM_LIMIT = 24 * 2**20


def whole_body(*args):
    n = lax.axis_size("tp")
    _, batch, ncols, dh = args[9].shape
    if n % 2 == 0 and ncols % 128 == 0 and dh % ncols == 0 and batch % (16 * CELL_CHUNKS) == 0:
        return fused_body(n, *args)
    return body(*args)


def solution(mesh):
    return jax.shard_map(
        whole_body,
        mesh=mesh,
        in_specs=(
            P("grp", None),
            P(),
            P(None, "tp", None),
            P(None, "tp", None),
            P(None, "tp", None),
            P(None, "tp", None),
            P(),
            P(),
            P(None, "tp", None),
            P(None, "grp", "tp", None),
            P(None, "grp", "tp"),
            P(None, "grp", None),
        ),
        out_specs=(
            P("grp", "tp"),
            P(None, "grp", "tp", None),
            P(None, "grp", "tp"),
            P(None, "grp", None),
        ),
        check_vma=False,
    )
```
